32 devices in a mesh: ep: 8 (over z, x), tp: 4 (over y, core).
Axes of the slice: x: 2, y: 2, z: 4, core: 2. Of those that a mesh axis runs over, the one named last changes fastest.
Arguments:
- conv_input: bfloat16 [4096, 2048], P(('ep', 'tp')), may hold values from -6 to 6
- conv_kernel: float32 [31, 2048], replicated, may hold values from -1 to 1
- conv_gain: float32 [2048], replicated, may hold values from 0.1 to 1.9
- out_weight: bfloat16 [2048, 2048], P(None, 'tp'), may hold values from -0.125 to 0.125
- moe_input: bfloat16 [4096, 2048], P(('ep', 'tp')), may hold values from -6 to 6
- moe_gain: float32 [2048], replicated, may hold values from 0.1 to 1.9
- expert_gate: bfloat16 [8, 2048, 2048], P('ep', None, 'tp'), may hold values from -0.125 to 0.125
- expert_up: bfloat16 [8, 2048, 2048], P('ep', None, 'tp'), may hold values from -0.125 to 0.125
- expert_down: bfloat16 [8, 2048, 2048], P('ep', 'tp'), may hold values from -0.125 to 0.125
- shared_gate: bfloat16 [2048, 128], replicated, may hold values from -0.125 to 0.125
- shared_up: bfloat16 [2048, 128], replicated, may hold values from -0.125 to 0.125
- shared_down: bfloat16 [128, 2048], replicated, may hold values from -0.5 to 0.5
- expert_index: int32 [4096, 2], P('ep'), may hold values from 0 to 7, all different within a row; in each aligned block of 128 rows (0 to 127, 128 to 255, ...) at most 48 rows name the same one
- routing_weight: float32 [4096, 2], P(('ep', 'tp')), may hold values from 0.25 to 1.5
Outputs:
- conv_out: bfloat16 [4096, 2048], P('ep', 'tp')
- moe_out: bfloat16 [4096, 2048], P(('ep', 'tp'))
The draws below stay inside these ranges and needn't reach their ends.
Inputs may be any that keep to these rules, and one draw needn't show every extreme that they name: `expert_index`: each row names 2 different experts. In each aligned block of 128 rows no expert is named by more than 48 of the rows, and in some blocks one expert is named by exactly 48 rows.
All inputs are finite; a program needn't handle non-finite values.
Results may differ from the reference program's by a relative error of at most 0.009.
Values may be sent and summed in bfloat16 or wider, within the bound.
A program may use at most 128 MiB of HBM per device.

```python
import math
import jax
import jax.numpy as jnp
import numpy as np
from jax import lax

D = 2048
FF = 2048
SHARED_FF = 128
TOPK = 2
KERNEL = 31
TOK_DEV_B = 128
TOKENS_A = 4096
TOKENS_B = 4096
EXPERTS = 8
SLOTS = 48
N_TP = 4


def level_of(key, dims, cuts, smallest, largest):
    def one(axis_at, blocks):
        heights = jax.random.uniform(jax.random.fold_in(jax.random.fold_in(key, 6), axis_at), (blocks,), jnp.float32, smallest / len(cuts), largest / len(cuts))
        return jnp.repeat(jnp.exp(heights), dims[axis_at] // blocks).reshape((-1,) + (1,) * (len(dims) - axis_at - 1))

    level = one(*cuts[0])
    for cut in cuts[1:]:
        level = level * one(*cut)
    return level


def shared_out(key, own, number, rows, number_of, top, limit, slope):
    sequence = jax.random.permutation(key, number_of)
    crowded, common = shares(number_of, rows * top, limit, slope, True), shares(number_of, rows * top, limit, slope, False)
    places = jnp.arange(number_of)

    def named(sizes, rotation):
        used = int((sizes > 0).sum())
        fixed = max(1, used // 4)
        moved = fixed + (places - fixed + rotation * (used - fixed)) % max(1, number_of - fixed)
        return jnp.zeros((number_of,), jnp.int32).at[sequence[jnp.where(places < fixed, places, moved)]].set(jnp.asarray(sizes, jnp.int32))

    sizes = jnp.where(number % 4 == 0, named(crowded, number // 4), named(common, number - number // 4 - 1))
    mixed = jax.random.permutation(jax.random.fold_in(own, 3), number_of)
    donor, receiver = mixed[0:number_of // 2 * 2:2], mixed[1:number_of // 2 * 2:2]
    slack = jnp.minimum(sizes[donor] - 1, limit - sizes[receiver]) // 2
    slack = jnp.where((donor == sequence[0]) | (receiver == sequence[0]) | (sizes[receiver] == 0), 0, jnp.maximum(slack, 0))
    moved = jax.random.randint(jax.random.fold_in(own, 4), (number_of // 2,), 0, 1 << 20) % (slack + 1)
    sizes = sizes.at[donor].add(-moved).at[receiver].add(moved)
    members = jnp.searchsorted(jnp.cumsum(sizes), jnp.arange(rows * top), side="right").astype(jnp.int32)
    grid = members.reshape(top, rows).T
    grid = grid[jax.random.permutation(jax.random.fold_in(own, 1), rows)]
    rotation = jax.random.randint(jax.random.fold_in(own, 2), (rows, 1), 0, top)
    return jnp.take_along_axis(grid, (jnp.arange(top)[None, :] + rotation) % top, axis=1)


def shares(count, total, bound, skew, full):
    weights = [(1 << 20) // math.isqrt(rank ** skew) + 1 for rank in range(1, count + 1)]
    largest = bound if full else min(bound, max(-(-total // count), total * weights[0] // sum(weights)))
    least = 1 if total - largest >= count - 1 else 0
    given, rest = [largest] + [least] * (count - 1), total - largest - least * (count - 1)
    while rest > 0:
        free = [i for i in range(1, count) if given[i] < largest] or [i for i in range(1, count) if given[i] < bound]
        pool, remaining = sum([weights[i] for i in free]), rest
        for i in free:
            addition = min(bound - given[i], max(1, remaining * weights[i] // pool), rest)
            given[i] = given[i] + addition
            rest = rest - addition
    return np.array(given)


def normal_values(key, extent, width, limit, split=(), kind=jnp.bfloat16):
    level = level_of(key, extent, split, -0.22, 0.18) if split else 1.0
    values = jax.random.normal(key, extent, jnp.float32) * width * level
    return jnp.minimum(jnp.maximum(values, -limit), limit).astype(kind)


def setup_inputs(seed: int = 0) -> dict:
    splits = jax.random.split(jax.random.key(seed), 15)
    conv_input = normal_values(splits[0], (TOKENS_A, D), 1.0, 6.0, ((0, 32),))
    conv_kernel = normal_values(splits[1], (KERNEL, D), KERNEL ** -0.5, 1.0, (), jnp.float32)
    conv_gain = jnp.clip(1.0 + 0.18 * jax.random.normal(splits[2], (D,), jnp.float32), 0.1, 1.9)
    out_weight = normal_values(splits[3], (D, D), D ** -0.5, 0.125, ((1, 4),))
    moe_input = normal_values(splits[4], (TOKENS_B, D), 1.0, 6.0, ((0, 32),))
    moe_gain = jnp.clip(1.0 + 0.18 * jax.random.normal(splits[5], (D,), jnp.float32), 0.1, 1.9)
    expert_gate = normal_values(splits[6], (EXPERTS, D, FF), D ** -0.5, 0.125, ((0, 8), (2, 4)))
    expert_up = normal_values(splits[7], (EXPERTS, D, FF), D ** -0.5, 0.125, ((0, 8), (2, 4)))
    expert_down = normal_values(splits[8], (EXPERTS, FF, D), FF ** -0.5, 0.125, ((0, 8), (1, 4)))
    shared_gate = normal_values(splits[9], (D, SHARED_FF), D ** -0.5, 0.125)
    shared_up = normal_values(splits[10], (D, SHARED_FF), D ** -0.5, 0.125)
    shared_down = normal_values(splits[11], (SHARED_FF, D), SHARED_FF ** -0.5, 0.5)
    expert_index_keys = jax.random.split(jax.random.fold_in(splits[12], 1), TOKENS_B // TOK_DEV_B)
    expert_index_turns = jax.random.permutation(jax.random.fold_in(splits[12], 3), TOKENS_B // TOK_DEV_B)
    expert_index = jax.vmap(lambda own, number: shared_out(jax.random.fold_in(splits[12], 2), own, number, TOK_DEV_B, EXPERTS, TOPK, SLOTS, 2))(expert_index_keys, expert_index_turns).reshape((TOKENS_B, TOPK))
    routing_weight = jnp.clip(0.25 + 1.25 * jax.random.uniform(splits[13], (TOKENS_B, TOPK), jnp.float32) ** level_of(splits[13], (TOKENS_B, TOPK), ((0, 32),), -0.2, 0.2), 0.25, 1.5)
    return dict(conv_input=conv_input, conv_kernel=conv_kernel, conv_gain=conv_gain, out_weight=out_weight, moe_input=moe_input, moe_gain=moe_gain, expert_gate=expert_gate, expert_up=expert_up, expert_down=expert_down, shared_gate=shared_gate, shared_up=shared_up, shared_down=shared_down, expert_index=expert_index, routing_weight=routing_weight)


NORM_EPS = 1e-05

def layer_scale(row_data, gain_vec):
    values = row_data.astype(jnp.float32)
    center = values - lax.optimization_barrier(jnp.mean(values, axis=-1, keepdims=True))
    spread = lax.optimization_barrier(jnp.mean(center * center, axis=-1, keepdims=True))
    return center * lax.rsqrt(spread + NORM_EPS) * gain_vec

def depthwise(padded, kernel, length):
    running = jnp.zeros((length, padded.shape[1]), jnp.float32)
    for offset in range(kernel.shape[0]):
        running = running + padded[offset:offset + length].astype(jnp.float32) * kernel[offset]
    return running

def slot_table(block_index, experts, slot_count):
    onehot = (block_index[:, :, None] == jnp.arange(experts, dtype=jnp.int32)[None, None, :]).astype(jnp.int32)
    before = jnp.cumsum(onehot, axis=1) - onehot
    position = lax.optimization_barrier(jnp.sum(before * onehot, axis=2))
    return (block_index * slot_count + position).astype(jnp.int32)

def reference(conv_input, conv_kernel, conv_gain, out_weight, moe_input, moe_gain, expert_gate, expert_up, expert_down, shared_gate, shared_up, shared_down, expert_index, routing_weight):
    length = conv_input.shape[0]
    padded = jnp.concatenate([jnp.zeros((KERNEL - 1, D), jnp.bfloat16), conv_input], axis=0)
    mixed_rows = depthwise(padded, conv_kernel, length)
    normed = jax.nn.silu(layer_scale(mixed_rows, conv_gain)).astype(jnp.bfloat16)
    conv_out = jnp.dot(normed, out_weight, preferred_element_type=jnp.float32).astype(jnp.bfloat16)
    normal = layer_scale(moe_input, moe_gain).astype(jnp.bfloat16)
    blocks = TOKENS_B // TOK_DEV_B
    entries = TOK_DEV_B * TOPK
    block_index = expert_index.reshape(blocks, entries)
    entry_slot = slot_table(block_index, EXPERTS, SLOTS)
    block_ids = jnp.arange(blocks, dtype=jnp.int32)[:, None]
    entry_row = block_ids * TOK_DEV_B + jnp.arange(entries, dtype=jnp.int32)[None, :] // TOPK
    slot_row = jnp.zeros((blocks, EXPERTS * SLOTS), jnp.int32).at[block_ids, entry_slot].set(entry_row)
    slot_weight = jnp.zeros((blocks, EXPERTS * SLOTS), jnp.float32).at[block_ids, entry_slot].set(routing_weight.reshape(blocks, entries))
    slot_row = slot_row.reshape(blocks, EXPERTS, SLOTS)
    slot_weight = slot_weight.reshape(blocks, EXPERTS, SLOTS)
    quarter = FF // N_TP

    def expert_step(running, expert_id):
        rows_of = lax.dynamic_index_in_dim(slot_row, expert_id, 1, keepdims=False).reshape(-1)
        weights = lax.dynamic_index_in_dim(slot_weight, expert_id, 1, keepdims=False).reshape(-1, 1)
        row_data = normal[rows_of]
        gate_proj = jnp.dot(row_data, expert_gate[expert_id], preferred_element_type=jnp.float32)
        up_proj = jnp.dot(row_data, expert_up[expert_id], preferred_element_type=jnp.float32)
        hidden = (jax.nn.silu(gate_proj) * up_proj).astype(jnp.bfloat16)
        down_all = expert_down[expert_id]
        summed = jnp.zeros((row_data.shape[0], D), jnp.float32)
        for index_q in range(N_TP):
            part_q = jnp.dot(hidden[:, index_q * quarter:(index_q + 1) * quarter], down_all[index_q * quarter:(index_q + 1) * quarter], preferred_element_type=jnp.float32).astype(jnp.bfloat16)
            summed = summed + lax.optimization_barrier(part_q).astype(jnp.float32)
        result = lax.optimization_barrier(summed.astype(jnp.bfloat16)).astype(jnp.float32)
        return (running.at[rows_of].add(weights * result), None)
    routed, _ = lax.scan(expert_step, jnp.zeros((TOKENS_B, D), jnp.float32), jnp.arange(EXPERTS, dtype=jnp.int32))
    shared_gate_proj = jnp.dot(normal, shared_gate, preferred_element_type=jnp.float32)
    shared_up_proj = jnp.dot(normal, shared_up, preferred_element_type=jnp.float32)
    shared_hidden = (jax.nn.silu(shared_gate_proj) * shared_up_proj).astype(jnp.bfloat16)
    shared_part = jnp.dot(shared_hidden, shared_down, preferred_element_type=jnp.float32)
    moe_out = (shared_part + routed).astype(jnp.bfloat16)
    return (conv_out, moe_out)
```

```python
import functools

import jax
import jax.numpy as jnp
from jax import lax
from jax.experimental import pallas as pl
from jax.experimental.pallas import tpu as pltpu
from jax.sharding import PartitionSpec as P

NORM_EPS = 1e-05


def passed_along(block, axis, distance):
    devices = range(lax.axis_size(axis))
    route = [(i - distance, i) for i in devices if i - distance in devices]
    return lax.ppermute(block, axis, route)


def layer_scale(row_data, gain_vec):
    values = row_data.astype(jnp.float32)
    center = values - jnp.mean(values, axis=-1, keepdims=True)
    spread = jnp.mean(center * center, axis=-1, keepdims=True)
    return center * lax.rsqrt(spread + NORM_EPS) * gain_vec


def depthwise(padded, kernel, length):
    running = jnp.zeros((length, padded.shape[1]), jnp.float32)
    for offset in range(kernel.shape[0]):
        running = running + padded[offset : offset + length].astype(jnp.float32) * kernel[offset]
    return running


def slot_table(block_index, experts, slot_count):
    onehot = (
        block_index[:, :, None] == jnp.arange(experts, dtype=jnp.int32)[None, None, :]
    ).astype(jnp.int32)
    before = jnp.cumsum(onehot, axis=1) - onehot
    position = jnp.sum(before * onehot, axis=2)
    return block_index * slot_count + position


def fill_slots(row_data, entry_slot, top_count, total_slots):
    block_count = entry_slot.shape[0]
    entries = entry_slot.shape[1]
    block_ids = jnp.arange(block_count, dtype=jnp.int32)[:, None]
    source = jnp.arange(entries, dtype=jnp.int32)[None, :] // top_count
    slot_row = (
        jnp.zeros((block_count, total_slots), jnp.int32).at[block_ids, entry_slot].set(source)
    )
    filled = jnp.zeros((block_count, total_slots), jnp.int32).at[block_ids, entry_slot].set(1)
    picked = row_data[block_ids, slot_row]
    return jnp.where(filled[:, :, None] > 0, picked, jnp.zeros((), row_data.dtype))


def gated(row_data, gate_weight, up_weight):
    gate_proj = jnp.dot(row_data, gate_weight, preferred_element_type=jnp.float32)
    up_proj = jnp.dot(row_data, up_weight, preferred_element_type=jnp.float32)
    return (jax.nn.silu(gate_proj) * up_proj).astype(jnp.bfloat16)


def on_device(
    conv_input,
    conv_kernel,
    conv_gain,
    out_weight,
    moe_input,
    moe_gain,
    expert_gate,
    expert_up,
    expert_down,
    shared_gate,
    shared_up,
    shared_down,
    expert_index,
    routing_weight,
):
    reach = conv_kernel.shape[0] - 1
    length = conv_input.shape[0]
    halo_rows = passed_along(conv_input[length - reach :], ("ep", "tp"), 1)
    padded = jnp.concatenate([halo_rows, conv_input], axis=0)
    mixed_rows = depthwise(padded, conv_kernel, length)
    normed = jax.nn.silu(layer_scale(mixed_rows, conv_gain)).astype(jnp.bfloat16)
    conv_out = jnp.dot(
        lax.all_gather(normed, "tp", axis=0, tiled=True),
        out_weight,
        preferred_element_type=jnp.float32,
    ).astype(jnp.bfloat16)
    tp_parts = lax.axis_size("tp")
    tp_index = lax.axis_index("tp")
    ep_ranks = lax.axis_size("ep")
    tok_count = moe_input.shape[0]
    top_count = routing_weight.shape[1]
    model_width = moe_input.shape[1]
    experts = ep_ranks * expert_gate.shape[0]
    slot_count = 3 * tok_count * top_count // (2 * experts)
    total_slots = experts * slot_count
    normal = layer_scale(moe_input, moe_gain).astype(jnp.bfloat16)
    group_slots = slot_table(
        expert_index.reshape(tp_parts, tok_count * top_count), experts, slot_count
    )
    own_slots = lax.dynamic_index_in_dim(group_slots, tp_index, 0, keepdims=True)
    gate_local = expert_gate[0]
    up_local = expert_up[0]
    down_local = expert_down[0]
    own_rows = fill_slots(normal[None], own_slots, top_count, total_slots)
    own_rows = own_rows.reshape(ep_ranks, slot_count, model_width)
    arrived = lax.all_to_all(own_rows, "ep", split_axis=0, concat_axis=0, tiled=True)
    hidden = gated(
        lax.all_gather(
            arrived.reshape(ep_ranks * slot_count, model_width), "tp", axis=0, tiled=True
        ),
        gate_local,
        up_local,
    )
    summed = lax.psum_scatter(
        jnp.dot(hidden, down_local, preferred_element_type=jnp.float32).astype(jnp.bfloat16),
        "tp",
        scatter_dimension=0,
        tiled=True,
    )
    returned = lax.all_to_all(
        summed.reshape(ep_ranks, slot_count, model_width),
        "ep",
        split_axis=0,
        concat_axis=0,
        tiled=True,
    )
    picked = returned.reshape(total_slots, model_width)[own_slots[0]]
    picked = picked.reshape(tok_count, top_count, model_width).astype(jnp.float32)
    routed = jnp.sum(picked * routing_weight[:, :, None], axis=1)
    shared_hidden = gated(normal, shared_gate, shared_up)
    shared_part = jnp.dot(shared_hidden, shared_down, preferred_element_type=jnp.float32)
    moe_out = (shared_part + routed).astype(jnp.bfloat16)
    return (conv_out, moe_out)


LANES = 128
ROW_TILE = 16
COLS = 512
MESH = pl.DeviceIdType.MESH


def fused_kernel(
    n,
    slots,
    reach,
    conv_in,
    taps,
    conv_gain,
    out_w_hbm,
    moe_in,
    moe_gain,
    gate_hbm,
    up_hbm,
    down_hbm,
    sh_gate,
    sh_up,
    sh_down,
    index_ref,
    weight_ref,
    conv_out,
    moe_out,
    own,
    gath,
    part,
    from_core,
    pair_sum,
    from_y,
    result,
    returned,
    normal,
    halo,
    pad,
    mixed,
    conv_all,
    gate_w,
    up_w,
    down_w,
    out_w,
    local_sem,
    chunk_send,
    chunk_recv,
    conv_send,
    conv_recv,
):
    tokens, width = moe_in.shape
    e = lax.axis_index("ep")
    t = lax.axis_index("tp")
    core = lax.rem(t, 2)
    row = t // 2
    core_peer = row * 2 + (1 - core)
    y_peer = (1 - row) * 2 + core
    diagonal = (1 - row) * 2 + (1 - core)
    place = e * 4 + t
    after = lax.rem(place + 1, n * 4)
    ahead = lax.rem(place + n * 4 - 1, n * 4)
    halo_rows = halo.shape[0]

    fetches = [
        pltpu.make_async_copy(src, dst, local_sem.at[i])
        for i, (src, dst) in enumerate(
            ((gate_hbm.at[0], gate_w), (up_hbm.at[0], up_w), (down_hbm.at[0], down_w), (out_w_hbm, out_w))
        )
    ]
    for fetch in fetches:
        fetch.start()

    barrier = pltpu.get_barrier_semaphore()
    greeted = [(lax.rem(e + k, n), t) for k in range(1, n)]
    greeted += [(e, core_peer), (e, y_peer)]
    greeted += [(after // 4, lax.rem(after, 4)), (ahead // 4, lax.rem(ahead, 4))]
    for device in greeted:
        pl.semaphore_signal(barrier, inc=1, device_id=device, device_id_type=MESH)
    pl.semaphore_wait(barrier, len(greeted))

    def remote(src, dst, kind, k, device):
        return pltpu.make_async_remote_copy(
            src_ref=src,
            dst_ref=dst,
            send_sem=chunk_send.at[kind, k],
            recv_sem=chunk_recv.at[kind, k],
            device_id=device,
            device_id_type=MESH,
        )

    def conv_copy(src, dst, kind, device):
        return pltpu.make_async_remote_copy(
            src_ref=src,
            dst_ref=dst,
            send_sem=conv_send.at[kind],
            recv_sem=conv_recv.at[kind],
            device_id=device,
            device_id_type=MESH,
        )

    def dispatch_copy(k):
        return remote(own.at[k], gath.at[k, t], 0, k, (lax.rem(e + k, n), t))

    def share_core(k, q):
        return remote(gath.at[k, q], gath.at[k, q], 1, k, (e, core_peer))

    def share_y(k, q):
        return remote(gath.at[k, q], gath.at[k, q], 2, k, (e, y_peer))

    def forward_core(k, q):
        return remote(gath.at[k, q], gath.at[k, q], 3, k, (e, core_peer))

    def reduce_core(k, q, which):
        return remote(part.at[k, q], from_core.at[which, k], 4 + which, k, (e, core_peer))

    def reduce_y(k):
        return remote(pair_sum.at[k], from_y.at[k], 6, k, (e, y_peer))

    def return_copy(k):
        return remote(result.at[k], returned.at[k], 7, k, (lax.rem(e - k + n, n), t))

    halo_copy = conv_copy(
        conv_in.at[pl.ds(tokens - halo_rows, halo_rows)],
        halo,
        0,
        (after // 4, lax.rem(after, 4)),
    )
    halo_copy.start()

    def normal_rows(i, carry):
        rows = pl.ds(pl.multiple_of(i * ROW_TILE, ROW_TILE), ROW_TILE)
        normal[rows, :] = layer_scale(moe_in[rows, :], moe_gain[...]).astype(jnp.bfloat16)
        return carry

    lax.fori_loop(0, tokens // ROW_TILE, normal_rows, 0)

    chosen = index_ref[pl.ds(pl.multiple_of(t * tokens, tokens), tokens), :]
    relative = chosen - e
    relative = jnp.where(relative < 0, relative + n, relative)
    first, second = relative[:, 0:1], relative[:, 1:2]
    lane = lax.broadcasted_iota(jnp.int32, (tokens, LANES), 1)
    hot_first = (lane == first).astype(jnp.float32)
    hot_second = (lane == second).astype(jnp.float32)
    earlier = (
        lax.broadcasted_iota(jnp.int32, (tokens, tokens), 0)
        > lax.broadcasted_iota(jnp.int32, (tokens, tokens), 1)
    ).astype(jnp.float32).astype(jnp.bfloat16)
    before = jnp.dot(
        earlier, (hot_first + hot_second).astype(jnp.bfloat16), preferred_element_type=jnp.float32
    )
    slot_first = first.astype(jnp.float32) * slots + jnp.sum(before * hot_first, axis=1, keepdims=True)
    slot_second = second.astype(jnp.float32) * slots + jnp.sum(
        before * hot_second, axis=1, keepdims=True
    )
    row_first = jnp.broadcast_to(slot_first, (tokens, LANES)).T[0:1, :]
    row_second = jnp.broadcast_to(slot_second, (tokens, LANES)).T[0:1, :]
    slot_row = lax.broadcasted_iota(jnp.int32, (n * slots, tokens), 0).astype(jnp.float32)
    spread = (
        jnp.where(slot_row == row_first, 1.0, 0.0) + jnp.where(slot_row == row_second, 1.0, 0.0)
    ).astype(jnp.bfloat16)
    for c in range(0, width, COLS):
        rows = jnp.dot(spread, normal[:, c : c + COLS], preferred_element_type=jnp.float32)
        rows = rows.astype(jnp.bfloat16).reshape(n, slots, COLS)
        own[:, :, c : c + COLS] = rows
        gath[0, t, :, c : c + COLS] = rows[0]

    for k in range(1, n):
        dispatch_copy(k).start()

    def relay(k):
        share_y(k, t).start()
        share_core(k, t).start()

    def forward(k):
        share_y(k, y_peer).wait_recv()
        forward_core(k, y_peer).start()

    relay(0)

    conv_copy(halo, halo, 0, (e, core_peer)).wait_recv()
    inside = jnp.where(place == 0, 0.0, 1.0)
    pad[0:halo_rows, :] = halo[...].astype(jnp.float32) * inside
    pad[halo_rows:, :] = conv_in[...].astype(jnp.float32)

    def strip(c, carry):
        cols = pl.ds(pl.multiple_of(c * LANES, LANES), LANES)
        total = jnp.zeros((tokens, LANES), jnp.float32)
        for k in range(reach + 1):
            start = halo_rows - reach + k
            total = total + pad[pl.ds(start, tokens), cols] * taps[pl.ds(k, 1), cols]
        mixed[:, cols] = total
        return carry

    lax.fori_loop(0, width // LANES, strip, 0)

    def conv_rows(i, carry):
        rows = pl.ds(pl.multiple_of(i * ROW_TILE, ROW_TILE), ROW_TILE)
        conv_all[t, rows, :] = jax.nn.silu(layer_scale(mixed[rows, :], conv_gain[...])).astype(
            jnp.bfloat16
        )
        return carry

    lax.fori_loop(0, tokens // ROW_TILE, conv_rows, 0)
    conv_y = conv_copy(conv_all.at[t], conv_all.at[t], 1, (e, y_peer))
    conv_core = conv_copy(conv_all.at[t], conv_all.at[t], 2, (e, core_peer))
    conv_pass = conv_copy(conv_all.at[y_peer], conv_all.at[y_peer], 3, (e, core_peer))
    conv_y.start()
    conv_core.start()

    dispatch_copy(1).wait_recv()
    relay(1)
    forward(0)
    for fetch in fetches[:3]:
        fetch.wait()

    def step(i, carry):
        @pl.when(i + 2 < n)
        def _():
            k = i + 2
            dispatch_copy(k).wait_recv()
            relay(k)

        @pl.when(i + 1 < n)
        def _():
            forward(i + 1)

        @pl.when(i == 2)
        def _():
            conv_copy(conv_all.at[y_peer], conv_all.at[y_peer], 1, (e, y_peer)).wait_recv()
            conv_pass.start()

        @pl.when(i < n)
        def _():
            share_core(i, core_peer).wait_recv()
            forward_core(i, diagonal).wait_recv()
            rows = gath[i].reshape(4 * slots, width)
            hidden = gated(rows, gate_w[...], up_w[...])
            for c in range(0, width, COLS):
                piece = jnp.dot(hidden, down_w[:, c : c + COLS], preferred_element_type=jnp.float32)
                part[i, :, :, c : c + COLS] = piece.astype(jnp.bfloat16).reshape(4, slots, COLS)
            reduce_core(i, diagonal, 1).start()
            reduce_core(i, core_peer, 0).start()

        @pl.when((i >= 1) & (i <= n))
        def _():
            k = i - 1
            reduce_core(k, core_peer, 1).wait_recv()
            pair_sum[k] = (
                part[k, y_peer].astype(jnp.float32) + from_core[1, k].astype(jnp.float32)
            ).astype(jnp.bfloat16)
            reduce_y(k).start()

        @pl.when(i >= 2)
        def _():
            k = i - 2
            reduce_core(k, core_peer, 0).wait_recv()
            reduce_y(k).wait_recv()
            total = part[k, t].astype(jnp.float32) + from_core[0, k].astype(jnp.float32)
            total = (total + from_y[k].astype(jnp.float32)).astype(jnp.bfloat16)

            @pl.when(k > 0)
            def _():
                result[k] = total
                return_copy(k).start()

            @pl.when(k == 0)
            def _():
                returned[0] = total

        return carry

    lax.fori_loop(0, n + 2, step, 0)

    conv_copy(conv_all.at[core_peer], conv_all.at[core_peer], 2, (e, core_peer)).wait_recv()
    conv_copy(conv_all.at[diagonal], conv_all.at[diagonal], 3, (e, core_peer)).wait_recv()
    fetches[3].wait()
    for q in range(4):
        conv_out[q * tokens : (q + 1) * tokens, :] = jnp.dot(
            conv_all[q], out_w[...], preferred_element_type=jnp.float32
        ).astype(jnp.bfloat16)

    shared = gated(normal[...], sh_gate[...], sh_up[...])
    slot_lane = lax.broadcasted_iota(jnp.int32, (tokens, n * slots), 1).astype(jnp.float32)
    share = jnp.where(slot_lane == slot_first, weight_ref[:, 0:1], 0.0) + jnp.where(
        slot_lane == slot_second, weight_ref[:, 1:2], 0.0
    )
    share_high = share.astype(jnp.bfloat16)
    share_low = (share - share_high.astype(jnp.float32)).astype(jnp.bfloat16)
    for k in range(1, n):
        return_copy(k).wait_recv()
    for c in range(0, width, COLS):
        rows = returned[:, :, c : c + COLS].reshape(n * slots, COLS)
        total = jnp.dot(shared, sh_down[:, c : c + COLS], preferred_element_type=jnp.float32)
        total = total + jnp.dot(share_high, rows, preferred_element_type=jnp.float32)
        total = total + jnp.dot(share_low, rows, preferred_element_type=jnp.float32)
        moe_out[:, c : c + COLS] = total.astype(jnp.bfloat16)

    halo_copy.wait_send()
    conv_y.wait_send()
    conv_core.wait_send()
    conv_pass.wait_send()

    def drain(k, carry):
        @pl.when(k > 0)
        def _():
            dispatch_copy(k).wait_send()
            return_copy(k).wait_send()

        share_y(k, t).wait_send()
        share_core(k, t).wait_send()
        forward_core(k, y_peer).wait_send()
        reduce_core(k, diagonal, 1).wait_send()
        reduce_core(k, core_peer, 0).wait_send()
        reduce_y(k).wait_send()
        return carry

    lax.fori_loop(0, n, drain, 0)


def fused(
    conv_input,
    conv_kernel,
    conv_gain,
    out_weight,
    moe_input,
    moe_gain,
    expert_gate,
    expert_up,
    expert_down,
    shared_gate,
    shared_up,
    shared_down,
    expert_index,
    routing_weight,
):
    n = lax.axis_size("ep")
    parts = lax.axis_size("tp")
    tokens, width = moe_input.shape
    slots = 3 * tokens * routing_weight.shape[1] // (2 * n)
    hidden = expert_gate.shape[2]
    reach = conv_kernel.shape[0] - 1
    halo_rows = -(-reach // ROW_TILE) * ROW_TILE
    out_cols = out_weight.shape[1]
    bf16 = jnp.bfloat16
    chunk = (n, slots, width)
    vmem = pl.BlockSpec(memory_space=pltpu.VMEM)
    hbm = pl.BlockSpec(memory_space=pl.ANY)
    return pl.pallas_call(
        functools.partial(fused_kernel, n, slots, reach),
        out_shape=(
            jax.ShapeDtypeStruct((parts * tokens, out_cols), bf16),
            jax.ShapeDtypeStruct((tokens, width), bf16),
        ),
        in_specs=[vmem, vmem, vmem, hbm, vmem, vmem, hbm, hbm, hbm, vmem, vmem, vmem, vmem, vmem],
        out_specs=(vmem, vmem),
        scratch_shapes=[
            pltpu.VMEM(chunk, bf16),
            pltpu.VMEM((n, parts, slots, width), bf16),
            pltpu.VMEM((n, parts, slots, width), bf16),
            pltpu.VMEM((2,) + chunk, bf16),
            pltpu.VMEM(chunk, bf16),
            pltpu.VMEM(chunk, bf16),
            pltpu.VMEM(chunk, bf16),
            pltpu.VMEM(chunk, bf16),
            pltpu.VMEM((tokens, width), bf16),
            pltpu.VMEM((halo_rows, width), bf16),
            pltpu.VMEM((halo_rows + tokens, width), jnp.float32),
            pltpu.VMEM((tokens, width), jnp.float32),
            pltpu.VMEM((parts, tokens, width), bf16),
            pltpu.VMEM((width, hidden), bf16),
            pltpu.VMEM((width, hidden), bf16),
            pltpu.VMEM((hidden, width), bf16),
            pltpu.VMEM((width, out_cols), bf16),
            pltpu.SemaphoreType.DMA((4,)),
            pltpu.SemaphoreType.DMA((8, n)),
            pltpu.SemaphoreType.DMA((8, n)),
            pltpu.SemaphoreType.DMA((4,)),
            pltpu.SemaphoreType.DMA((4,)),
        ],
        compiler_params=pltpu.CompilerParams(
            collective_id=0, has_side_effects=True, vmem_limit_bytes=60 * 1024 * 1024
        ),
    )(
        conv_input,
        conv_kernel,
        conv_gain.reshape(1, width),
        out_weight,
        moe_input,
        moe_gain.reshape(1, width),
        expert_gate,
        expert_up,
        expert_down,
        shared_gate,
        shared_up,
        shared_down,
        expert_index,
        routing_weight,
    )


def fits_fused(args):
    n, parts = lax.axis_size("ep"), lax.axis_size("tp")
    conv_input, conv_kernel, moe_input = args[0], args[1], args[4]
    top_count = args[13].shape[1]
    tokens, width = moe_input.shape
    slots = 3 * tokens * top_count // (2 * n)
    return (
        parts == 4
        and top_count == 2
        and args[6].shape[0] == 1
        and conv_input.shape == moe_input.shape
        and conv_kernel.shape[0] - 1 <= tokens
        and tokens % LANES == 0
        and width % COLS == 0
        and slots % ROW_TILE == 0
        and slots >= ROW_TILE
        and n <= LANES
    )


def either(*args):
    return fused(*args) if fits_fused(args) else on_device(*args)


def solution(mesh):
    in_specs = (
        P(("ep", "tp"), None),
        P(),
        P(),
        P(None, "tp"),
        P(("ep", "tp"), None),
        P(),
        P("ep", None, "tp"),
        P("ep", None, "tp"),
        P("ep", "tp", None),
        P(),
        P(),
        P(),
        P("ep", None),
        P(("ep", "tp"), None),
    )
    out_specs = (P("ep", "tp"), P(("ep", "tp"), None))
    return jax.shard_map(
        either, mesh=mesh, in_specs=in_specs, out_specs=out_specs, check_vma=False
    )
```

```python
import functools

import jax
import jax.numpy as jnp
from jax import lax
from jax.experimental import pallas as pl
from jax.experimental.pallas import tpu as pltpu
from jax.sharding import PartitionSpec as P

NORM_EPS = 1e-05


def passed_along(block, axis, distance):
    devices = range(lax.axis_size(axis))
    route = [(i - distance, i) for i in devices if i - distance in devices]
    return lax.ppermute(block, axis, route)


def layer_scale(row_data, gain_vec):
    values = row_data.astype(jnp.float32)
    center = values - jnp.mean(values, axis=-1, keepdims=True)
    spread = jnp.mean(center * center, axis=-1, keepdims=True)
    return center * lax.rsqrt(spread + NORM_EPS) * gain_vec


def depthwise(padded, kernel, length):
    running = jnp.zeros((length, padded.shape[1]), jnp.float32)
    for offset in range(kernel.shape[0]):
        running = running + padded[offset : offset + length].astype(jnp.float32) * kernel[offset]
    return running


def slot_table(block_index, experts, slot_count):
    onehot = (
        block_index[:, :, None] == jnp.arange(experts, dtype=jnp.int32)[None, None, :]
    ).astype(jnp.int32)
    before = jnp.cumsum(onehot, axis=1) - onehot
    position = jnp.sum(before * onehot, axis=2)
    return block_index * slot_count + position


def fill_slots(row_data, entry_slot, top_count, total_slots):
    block_count = entry_slot.shape[0]
    entries = entry_slot.shape[1]
    block_ids = jnp.arange(block_count, dtype=jnp.int32)[:, None]
    source = jnp.arange(entries, dtype=jnp.int32)[None, :] // top_count
    slot_row = (
        jnp.zeros((block_count, total_slots), jnp.int32).at[block_ids, entry_slot].set(source)
    )
    filled = jnp.zeros((block_count, total_slots), jnp.int32).at[block_ids, entry_slot].set(1)
    picked = row_data[block_ids, slot_row]
    return jnp.where(filled[:, :, None] > 0, picked, jnp.zeros((), row_data.dtype))


def gated(row_data, gate_weight, up_weight):
    gate_proj = jnp.dot(row_data, gate_weight, preferred_element_type=jnp.float32)
    up_proj = jnp.dot(row_data, up_weight, preferred_element_type=jnp.float32)
    return (jax.nn.silu(gate_proj) * up_proj).astype(jnp.bfloat16)


def on_device(
    conv_input,
    conv_kernel,
    conv_gain,
    out_weight,
    moe_input,
    moe_gain,
    expert_gate,
    expert_up,
    expert_down,
    shared_gate,
    shared_up,
    shared_down,
    expert_index,
    routing_weight,
):
    reach = conv_kernel.shape[0] - 1
    length = conv_input.shape[0]
    halo_rows = passed_along(conv_input[length - reach :], ("ep", "tp"), 1)
    padded = jnp.concatenate([halo_rows, conv_input], axis=0)
    mixed_rows = depthwise(padded, conv_kernel, length)
    normed = jax.nn.silu(layer_scale(mixed_rows, conv_gain)).astype(jnp.bfloat16)
    conv_out = jnp.dot(
        lax.all_gather(normed, "tp", axis=0, tiled=True),
        out_weight,
        preferred_element_type=jnp.float32,
    ).astype(jnp.bfloat16)
    tp_parts = lax.axis_size("tp")
    tp_index = lax.axis_index("tp")
    ep_ranks = lax.axis_size("ep")
    tok_count = moe_input.shape[0]
    top_count = routing_weight.shape[1]
    model_width = moe_input.shape[1]
    experts = ep_ranks * expert_gate.shape[0]
    slot_count = 3 * tok_count * top_count // (2 * experts)
    total_slots = experts * slot_count
    normal = layer_scale(moe_input, moe_gain).astype(jnp.bfloat16)
    group_slots = slot_table(
        expert_index.reshape(tp_parts, tok_count * top_count), experts, slot_count
    )
    own_slots = lax.dynamic_index_in_dim(group_slots, tp_index, 0, keepdims=True)
    gate_local = expert_gate[0]
    up_local = expert_up[0]
    down_local = expert_down[0]
    own_rows = fill_slots(normal[None], own_slots, top_count, total_slots)
    own_rows = own_rows.reshape(ep_ranks, slot_count, model_width)
    arrived = lax.all_to_all(own_rows, "ep", split_axis=0, concat_axis=0, tiled=True)
    hidden = gated(
        lax.all_gather(
            arrived.reshape(ep_ranks * slot_count, model_width), "tp", axis=0, tiled=True
        ),
        gate_local,
        up_local,
    )
    summed = lax.psum_scatter(
        jnp.dot(hidden, down_local, preferred_element_type=jnp.float32).astype(jnp.bfloat16),
        "tp",
        scatter_dimension=0,
        tiled=True,
    )
    returned = lax.all_to_all(
        summed.reshape(ep_ranks, slot_count, model_width),
        "ep",
        split_axis=0,
        concat_axis=0,
        tiled=True,
    )
    picked = returned.reshape(total_slots, model_width)[own_slots[0]]
    picked = picked.reshape(tok_count, top_count, model_width).astype(jnp.float32)
    routed = jnp.sum(picked * routing_weight[:, :, None], axis=1)
    shared_hidden = gated(normal, shared_gate, shared_up)
    shared_part = jnp.dot(shared_hidden, shared_down, preferred_element_type=jnp.float32)
    moe_out = (shared_part + routed).astype(jnp.bfloat16)
    return (conv_out, moe_out)


LANES = 128
ROW_TILE = 16
COLS = 512
MESH = pl.DeviceIdType.MESH


def fused_kernel(
    n,
    slots,
    reach,
    conv_in,
    taps,
    conv_gain,
    out_w_hbm,
    moe_in,
    moe_gain,
    gate_hbm,
    up_hbm,
    down_hbm,
    sh_gate,
    sh_up,
    sh_down,
    index_ref,
    weight_ref,
    conv_out,
    moe_out,
    own,
    gath,
    part,
    from_core,
    pair_sum,
    from_y,
    result,
    returned,
    normal,
    halo,
    pad,
    mixed,
    conv_all,
    gate_w,
    up_w,
    down_w,
    out_w,
    local_sem,
    chunk_send,
    chunk_recv,
    conv_send,
    conv_recv,
):
    tokens, width = moe_in.shape
    e = lax.axis_index("ep")
    t = lax.axis_index("tp")
    core = lax.rem(t, 2)
    row = t // 2
    core_peer = row * 2 + (1 - core)
    y_peer = (1 - row) * 2 + core
    diagonal = (1 - row) * 2 + (1 - core)
    place = e * 4 + t
    after = lax.rem(place + 1, n * 4)
    ahead = lax.rem(place + n * 4 - 1, n * 4)
    halo_rows = halo.shape[0]
    half = n // 2

    fetches = [
        pltpu.make_async_copy(src, dst, local_sem.at[i])
        for i, (src, dst) in enumerate(
            ((gate_hbm.at[0], gate_w), (up_hbm.at[0], up_w), (down_hbm.at[0], down_w), (out_w_hbm, out_w))
        )
    ]
    for fetch in fetches:
        fetch.start()

    barrier = pltpu.get_barrier_semaphore()
    greeted = [(lax.rem(e + k, n), t) for k in range(1, n)]
    greeted += [(e, core_peer), (e, y_peer)]
    greeted += [(after // 4, lax.rem(after, 4)), (ahead // 4, lax.rem(ahead, 4))]
    for device in greeted:
        pl.semaphore_signal(barrier, inc=1, device_id=device, device_id_type=MESH)
    pl.semaphore_wait(barrier, len(greeted))

    def remote(src, dst, kind, k, device):
        return pltpu.make_async_remote_copy(
            src_ref=src,
            dst_ref=dst,
            send_sem=chunk_send.at[kind, k],
            recv_sem=chunk_recv.at[kind, k],
            device_id=device,
            device_id_type=MESH,
        )

    def conv_copy(src, dst, kind, device):
        return pltpu.make_async_remote_copy(
            src_ref=src,
            dst_ref=dst,
            send_sem=conv_send.at[kind],
            recv_sem=conv_recv.at[kind],
            device_id=device,
            device_id_type=MESH,
        )

    def hop(k):
        odd = lax.rem(k, 2)
        return odd * (half + k // 2) + (1 - odd) * lax.rem(half - k // 2, half)

    def dispatch_copy(k):
        return remote(own.at[k], gath.at[k, t], 0, k, (lax.rem(e + hop(k), n), t))

    def share_core(k, q):
        return remote(gath.at[k, q], gath.at[k, q], 1, k, (e, core_peer))

    def share_y(k, q):
        return remote(gath.at[k, q], gath.at[k, q], 2, k, (e, y_peer))

    def forward_core(k, q):
        return remote(gath.at[k, q], gath.at[k, q], 3, k, (e, core_peer))

    def reduce_core(k, q, which):
        return remote(part.at[k, q], from_core.at[which, k], 4 + which, k, (e, core_peer))

    def reduce_y(k):
        return remote(pair_sum.at[k], from_y.at[k], 6, k, (e, y_peer))

    def return_copy(k):
        return remote(result.at[k], returned.at[k], 7, k, (lax.rem(e - hop(k) + n, n), t))

    halo_copy = conv_copy(
        conv_in.at[pl.ds(tokens - halo_rows, halo_rows)],
        halo,
        0,
        (after // 4, lax.rem(after, 4)),
    )
    halo_copy.start()

    def normal_rows(i, carry):
        rows = pl.ds(pl.multiple_of(i * ROW_TILE, ROW_TILE), ROW_TILE)
        normal[rows, :] = layer_scale(moe_in[rows, :], moe_gain[...]).astype(jnp.bfloat16)
        return carry

    lax.fori_loop(0, tokens // ROW_TILE, normal_rows, 0)

    def column(row_data):
        return jnp.broadcast_to(row_data, (LANES, tokens)).T[:, 0:1]

    chosen = index_ref[:, pl.ds(pl.multiple_of(t * tokens, tokens), tokens)]
    relative = chosen - e
    relative = jnp.where(relative < 0, relative + n, relative)
    order = jnp.where(relative >= half, 2 * (relative - half) + 1, 2 * (half - relative))
    order = jnp.where(order == n, 0, order).astype(jnp.float32)
    first, second = column(order[0:1, :]), column(order[1:2, :])
    lane = lax.broadcasted_iota(jnp.int32, (tokens, LANES), 1).astype(jnp.float32)
    hot_first = (lane == first).astype(jnp.float32)
    hot_second = (lane == second).astype(jnp.float32)
    earlier = (
        lax.broadcasted_iota(jnp.int32, (tokens, tokens), 0)
        > lax.broadcasted_iota(jnp.int32, (tokens, tokens), 1)
    ).astype(jnp.float32).astype(jnp.bfloat16)
    before = jnp.dot(
        earlier, (hot_first + hot_second).astype(jnp.bfloat16), preferred_element_type=jnp.float32
    )
    slot_first = first * slots + jnp.sum(before * hot_first, axis=1, keepdims=True)
    slot_second = second * slots + jnp.sum(
        before * hot_second, axis=1, keepdims=True
    )
    row_first = jnp.broadcast_to(slot_first, (tokens, LANES)).T[0:1, :]
    row_second = jnp.broadcast_to(slot_second, (tokens, LANES)).T[0:1, :]
    slot_row = lax.broadcasted_iota(jnp.int32, (n * slots, tokens), 0).astype(jnp.float32)
    spread = (
        jnp.where(slot_row == row_first, 1.0, 0.0) + jnp.where(slot_row == row_second, 1.0, 0.0)
    ).astype(jnp.bfloat16)
    for c in range(0, width, COLS):
        rows = jnp.dot(spread, normal[:, c : c + COLS], preferred_element_type=jnp.float32)
        rows = rows.astype(jnp.bfloat16).reshape(n, slots, COLS)
        own[:, :, c : c + COLS] = rows
        gath[0, t, :, c : c + COLS] = rows[0]

    for k in range(1, n):
        dispatch_copy(k).start()

    def relay(k):
        share_y(k, t).start()
        share_core(k, t).start()

    def forward(k):
        share_y(k, y_peer).wait_recv()
        forward_core(k, y_peer).start()

    relay(0)

    conv_copy(halo, halo, 0, (e, core_peer)).wait_recv()
    inside = jnp.where(place == 0, 0.0, 1.0)
    pad[0:halo_rows, :] = halo[...].astype(jnp.float32) * inside
    pad[halo_rows:, :] = conv_in[...].astype(jnp.float32)

    def strip(c, carry):
        cols = pl.ds(pl.multiple_of(c * LANES, LANES), LANES)
        total = jnp.zeros((tokens, LANES), jnp.float32)
        for k in range(reach + 1):
            start = halo_rows - reach + k
            total = total + pad[pl.ds(start, tokens), cols] * taps[pl.ds(k, 1), cols]
        mixed[:, cols] = total
        return carry

    lax.fori_loop(0, width // LANES, strip, 0)

    def conv_rows(i, carry):
        rows = pl.ds(pl.multiple_of(i * ROW_TILE, ROW_TILE), ROW_TILE)
        conv_all[t, rows, :] = jax.nn.silu(layer_scale(mixed[rows, :], conv_gain[...])).astype(
            jnp.bfloat16
        )
        return carry

    lax.fori_loop(0, tokens // ROW_TILE, conv_rows, 0)
    conv_y = conv_copy(conv_all.at[t], conv_all.at[t], 1, (e, y_peer))
    conv_core = conv_copy(conv_all.at[t], conv_all.at[t], 2, (e, core_peer))
    conv_pass = conv_copy(conv_all.at[y_peer], conv_all.at[y_peer], 3, (e, core_peer))
    conv_y.start()
    conv_core.start()

    dispatch_copy(1).wait_recv()
    relay(1)
    forward(0)
    for fetch in fetches[:3]:
        fetch.wait()

    def step(i, carry):
        @pl.when(i + 2 < n)
        def _():
            k = i + 2
            dispatch_copy(k).wait_recv()
            relay(k)

        @pl.when(i + 1 < n)
        def _():
            forward(i + 1)

        @pl.when(i == 2)
        def _():
            conv_copy(conv_all.at[y_peer], conv_all.at[y_peer], 1, (e, y_peer)).wait_recv()
            conv_pass.start()

        @pl.when(i < n)
        def _():
            share_core(i, core_peer).wait_recv()
            forward_core(i, diagonal).wait_recv()
            rows = gath[i].reshape(4 * slots, width)
            hidden = gated(rows, gate_w[...], up_w[...])
            for c in range(0, width, COLS):
                piece = jnp.dot(hidden, down_w[:, c : c + COLS], preferred_element_type=jnp.float32)
                part[i, :, :, c : c + COLS] = piece.astype(jnp.bfloat16).reshape(4, slots, COLS)
            reduce_core(i, diagonal, 1).start()
            reduce_core(i, core_peer, 0).start()

        @pl.when((i >= 1) & (i <= n))
        def _():
            k = i - 1
            reduce_core(k, core_peer, 1).wait_recv()
            pair_sum[k] = (
                part[k, y_peer].astype(jnp.float32) + from_core[1, k].astype(jnp.float32)
            ).astype(jnp.bfloat16)
            reduce_y(k).start()

        @pl.when(i >= 2)
        def _():
            k = i - 2
            reduce_core(k, core_peer, 0).wait_recv()
            reduce_y(k).wait_recv()
            total = part[k, t].astype(jnp.float32) + from_core[0, k].astype(jnp.float32)
            total = (total + from_y[k].astype(jnp.float32)).astype(jnp.bfloat16)

            @pl.when(k > 0)
            def _():
                result[k] = total
                return_copy(k).start()

            @pl.when(k == 0)
            def _():
                returned[0] = total

        return carry

    lax.fori_loop(0, n + 2, step, 0)

    conv_copy(conv_all.at[core_peer], conv_all.at[core_peer], 2, (e, core_peer)).wait_recv()
    conv_copy(conv_all.at[diagonal], conv_all.at[diagonal], 3, (e, core_peer)).wait_recv()
    fetches[3].wait()
    for q in range(4):
        conv_out[q * tokens : (q + 1) * tokens, :] = jnp.dot(
            conv_all[q], out_w[...], preferred_element_type=jnp.float32
        ).astype(jnp.bfloat16)

    shared = gated(normal[...], sh_gate[...], sh_up[...])
    slot_lane = lax.broadcasted_iota(jnp.int32, (tokens, n * slots), 1).astype(jnp.float32)
    share = jnp.where(slot_lane == slot_first, column(weight_ref[0:1, :]), 0.0) + jnp.where(
        slot_lane == slot_second, column(weight_ref[1:2, :]), 0.0
    )
    share_high = share.astype(jnp.bfloat16)
    share_low = (share - share_high.astype(jnp.float32)).astype(jnp.bfloat16)
    for k in range(1, n):
        return_copy(k).wait_recv()
    for c in range(0, width, COLS):
        rows = returned[:, :, c : c + COLS].reshape(n * slots, COLS)
        total = jnp.dot(shared, sh_down[:, c : c + COLS], preferred_element_type=jnp.float32)
        total = total + jnp.dot(share_high, rows, preferred_element_type=jnp.float32)
        total = total + jnp.dot(share_low, rows, preferred_element_type=jnp.float32)
        moe_out[:, c : c + COLS] = total.astype(jnp.bfloat16)

    halo_copy.wait_send()
    conv_y.wait_send()
    conv_core.wait_send()
    conv_pass.wait_send()

    def drain(k, carry):
        @pl.when(k > 0)
        def _():
            dispatch_copy(k).wait_send()
            return_copy(k).wait_send()

        share_y(k, t).wait_send()
        share_core(k, t).wait_send()
        forward_core(k, y_peer).wait_send()
        reduce_core(k, diagonal, 1).wait_send()
        reduce_core(k, core_peer, 0).wait_send()
        reduce_y(k).wait_send()
        return carry

    lax.fori_loop(0, n, drain, 0)


def fused(
    conv_input,
    conv_kernel,
    conv_gain,
    out_weight,
    moe_input,
    moe_gain,
    expert_gate,
    expert_up,
    expert_down,
    shared_gate,
    shared_up,
    shared_down,
    expert_index,
    routing_weight,
):
    n = lax.axis_size("ep")
    parts = lax.axis_size("tp")
    tokens, width = moe_input.shape
    slots = 3 * tokens * routing_weight.shape[1] // (2 * n)
    hidden = expert_gate.shape[2]
    reach = conv_kernel.shape[0] - 1
    halo_rows = -(-reach // ROW_TILE) * ROW_TILE
    out_cols = out_weight.shape[1]
    bf16 = jnp.bfloat16
    chunk = (n, slots, width)
    vmem = pl.BlockSpec(memory_space=pltpu.VMEM)
    hbm = pl.BlockSpec(memory_space=pl.ANY)
    return pl.pallas_call(
        functools.partial(fused_kernel, n, slots, reach),
        out_shape=(
            jax.ShapeDtypeStruct((parts * tokens, out_cols), bf16),
            jax.ShapeDtypeStruct((tokens, width), bf16),
        ),
        in_specs=[vmem, vmem, vmem, hbm, vmem, vmem, hbm, hbm, hbm, vmem, vmem, vmem, vmem, vmem],
        out_specs=(vmem, vmem),
        scratch_shapes=[
            pltpu.VMEM(chunk, bf16),
            pltpu.VMEM((n, parts, slots, width), bf16),
            pltpu.VMEM((n, parts, slots, width), bf16),
            pltpu.VMEM((2,) + chunk, bf16),
            pltpu.VMEM(chunk, bf16),
            pltpu.VMEM(chunk, bf16),
            pltpu.VMEM(chunk, bf16),
            pltpu.VMEM(chunk, bf16),
            pltpu.VMEM((tokens, width), bf16),
            pltpu.VMEM((halo_rows, width), bf16),
            pltpu.VMEM((halo_rows + tokens, width), jnp.float32),
            pltpu.VMEM((tokens, width), jnp.float32),
            pltpu.VMEM((parts, tokens, width), bf16),
            pltpu.VMEM((width, hidden), bf16),
            pltpu.VMEM((width, hidden), bf16),
            pltpu.VMEM((hidden, width), bf16),
            pltpu.VMEM((width, out_cols), bf16),
            pltpu.SemaphoreType.DMA((4,)),
            pltpu.SemaphoreType.DMA((8, n)),
            pltpu.SemaphoreType.DMA((8, n)),
            pltpu.SemaphoreType.DMA((4,)),
            pltpu.SemaphoreType.DMA((4,)),
        ],
        compiler_params=pltpu.CompilerParams(
            collective_id=0, has_side_effects=True, vmem_limit_bytes=60 * 1024 * 1024
        ),
    )(
        conv_input,
        conv_kernel,
        conv_gain.reshape(1, width),
        out_weight,
        moe_input,
        moe_gain.reshape(1, width),
        expert_gate,
        expert_up,
        expert_down,
        shared_gate,
        shared_up,
        shared_down,
        expert_index.T,
        routing_weight.T,
    )


def fits_fused(args):
    n, parts = lax.axis_size("ep"), lax.axis_size("tp")
    conv_input, conv_kernel, moe_input = args[0], args[1], args[4]
    top_count = args[13].shape[1]
    tokens, width = moe_input.shape
    slots = 3 * tokens * top_count // (2 * n)
    return (
        parts == 4
        and top_count == 2
        and args[6].shape[0] == 1
        and conv_input.shape == moe_input.shape
        and conv_kernel.shape[0] - 1 <= tokens
        and tokens % LANES == 0
        and width % COLS == 0
        and slots % ROW_TILE == 0
        and slots >= ROW_TILE
        and n <= LANES
        and n % 2 == 0
    )


def either(*args):
    return fused(*args) if fits_fused(args) else on_device(*args)


def solution(mesh):
    in_specs = (
        P(("ep", "tp"), None),
        P(),
        P(),
        P(None, "tp"),
        P(("ep", "tp"), None),
        P(),
        P("ep", None, "tp"),
        P("ep", None, "tp"),
        P("ep", "tp", None),
        P(),
        P(),
        P(),
        P("ep", None),
        P(("ep", "tp"), None),
    )
    out_specs = (P("ep", "tp"), P(("ep", "tp"), None))
    return jax.shard_map(
        either, mesh=mesh, in_specs=in_specs, out_specs=out_specs, check_vma=False
    )
```
